32 devices in a mesh: sp: 16 (over z, y, x), tp: 2 (over core).
Axes of the slice: x: 2, y: 2, z: 4, core: 2. Of those that a mesh axis runs over, the one named last changes fastest.
Arguments:
- tokens: bfloat16 [4096, 4096], P('sp', 'tp'), may hold values from -480 to 480
- gain: float32 [4096], P('tp'), may hold values from 0.1 to 1.9
- q_att: bfloat16 [4096, 2048], P('sp', 'tp'), may hold values from -2.90625 to 2.90625
- k_att: bfloat16 [4096, 1024], P('sp', 'tp'), may hold values from -0.09375 to 0.09375
- v_att: bfloat16 [4096, 1024], P('sp', 'tp'), may hold values from -0.75 to 0.75
- q_ret: bfloat16 [4096, 1024], P('sp', 'tp'), may hold values from -0.09375 to 0.09375
- k_ret: bfloat16 [4096, 1024], P('sp', 'tp'), may hold values from -0.09375 to 0.09375
- v_ret: bfloat16 [4096, 1024], P('sp', 'tp'), may hold values from -0.09375 to 0.09375
- out_att: bfloat16 [2048, 4096], P('tp', 'sp'), may hold values from -0.109375 to 0.109375
- out_ret: bfloat16 [1024, 4096], P('tp', 'sp'), may hold values from -0.109375 to 0.109375
- sink: float32 [16], P('tp'), may hold values from 3 to 7
- decay_log: float32 [8, 4096], P('tp', 'sp'), may hold values from -2.125 to 0
Outputs:
- mixed: bfloat16 [4096, 4096], P(('sp', 'tp'))
- log_weight: float32 [16, 4096], P('tp', 'sp')
The draws below stay inside these ranges and needn't reach their ends.
All inputs are finite; a program needn't handle non-finite values.
Results may differ from the reference program's by a relative error of at most 0.017.
Values may be sent and summed in bfloat16 or wider, within the bound.
No kernel may reach another device: no remote copies, remote signals or barrier semaphores. Data moves between devices by JAX's collectives and lax.ppermute only.
A program may use at most 128 MiB of HBM per device.

```python
import jax
import jax.numpy as jnp
from jax import lax

D = 4096
ATT_HEADS = 16
KV_HEADS = 8
RET_HEADS = 8
HEAD_DIM = 128
SPAN_RADIUS = 128
TOK_DEV = 256
TOKENS = 4096
N_TP = 2


def drawn_pair(key):
    base = jax.random.fold_in(key, 31)
    lookup_fraction = jnp.clip(jax.random.normal(jax.random.fold_in(base, 1), (D, KV_HEADS * HEAD_DIM), jnp.float32), -6.0, 6.0) * D ** (-0.5)
    query_part = jnp.clip(jax.random.normal(jax.random.fold_in(base, 2), (D, ATT_HEADS * HEAD_DIM), jnp.float32), -6.0, 6.0) * D ** (-0.5)
    return (query_part, lookup_fraction)


def draw_q_att(key, part):
    return drawn_pair(key)[0].astype(jnp.bfloat16)


def draw_k_att(key, part):
    return drawn_pair(key)[1].astype(jnp.bfloat16)


def draw_tokens(key, part):
    normal_part = jnp.clip(jax.random.normal(jax.random.fold_in(key, 41), (TOKENS, D), jnp.float32), -6.0, 6.0)
    column = jnp.arange(D).astype(jnp.float32) / D
    course = 2.0 * (jnp.arange(TOKENS).astype(jnp.float32) + 0.5) / TOKENS - 1.0
    direction = jax.random.uniform(jax.random.fold_in(key, 43), (1, D), jnp.float32, -1.0, 1.0)
    drift = jnp.exp(1.2 * direction * course[:, None])
    scale = drift * (4.0 ** column)[None, :]
    return (normal_part * scale).astype(jnp.bfloat16)


def draw_decay_log(key, part):
    blocks = TOKENS // TOK_DEV
    share = 0.5
    fast = jax.random.uniform(jax.random.fold_in(key, 51), (RET_HEADS, 1), jnp.float32) < share
    fast_rate = jax.random.uniform(jax.random.fold_in(key, 52), (RET_HEADS, 1), jnp.float32, 10.0, 16.0) / TOK_DEV
    slow_rate = jax.random.uniform(jax.random.fold_in(key, 53), (RET_HEADS, 1), jnp.float32, 0.1, 0.3) / TOKENS
    fading_pace = jnp.where(fast, fast_rate, slow_rate)
    scaling_factor = jnp.exp(jax.random.uniform(jax.random.fold_in(key, 54), (RET_HEADS, blocks), jnp.float32, jnp.log(0.5), jnp.log(2.0)))
    scaling_factor = jnp.repeat(scaling_factor, TOK_DEV, axis=1)
    spots = jax.random.randint(jax.random.fold_in(key, 55), (2,), 0, TOKENS)
    agreement_tally = (jnp.arange(TOKENS)[None, :] == spots[:, None]).astype(jnp.float32)
    discarded_entries = jnp.log(jax.random.uniform(jax.random.fold_in(key, 56), (2, RET_HEADS), jnp.float32, 0.5, 0.8))
    clustered_lists = jnp.dot(discarded_entries.T, agreement_tally)
    return -fading_pace * scaling_factor + clustered_lists


def steps_of(key, dims, cuts, least, largest):
    loudness, own = 1.0, jax.random.fold_in(key, 6)
    for axis_at, shards_of in cuts:
        heights = jnp.exp(jax.random.uniform(jax.random.fold_in(own, axis_at), (shards_of,), jnp.float32, least / len(cuts), largest / len(cuts)))
        loudness = loudness * jnp.repeat(heights, dims[axis_at] // shards_of).reshape([-1 if axis == axis_at else 1 for axis in range(len(dims))])
    return loudness


def scatter_about(key, extent, spread, reach, split=(), kind=jnp.bfloat16):
    values = jax.random.normal(key, extent, jnp.float32) * spread
    if len(split) > 0:
        values = steps_of(key, extent, split, -0.22, 0.18) * values
    return jnp.clip(values, min=-reach, max=reach).astype(kind)


def setup_inputs(seed: int = 0) -> dict:
    streams_of = jax.random.split(jax.random.key(seed), 13)
    return {
        "tokens": draw_tokens(jax.random.fold_in(streams_of[12], 71), 0),
        "gain": jnp.clip(1.0 + 0.18 * jax.random.normal(streams_of[1], (D,), jnp.float32), 0.1, 1.9),
        "q_att": draw_q_att(jax.random.fold_in(streams_of[12], 71), 0),
        "k_att": draw_k_att(jax.random.fold_in(streams_of[12], 71), 0),
        "v_att": scatter_about(streams_of[4], (D, KV_HEADS * HEAD_DIM), (max(D // 64, 1)) ** -0.5, 0.75, ((0, 16), (1, 2))),
        "q_ret": scatter_about(streams_of[5], (D, RET_HEADS * HEAD_DIM), D ** -0.5, 0.09375, ((0, 16), (1, 2))),
        "k_ret": scatter_about(streams_of[6], (D, RET_HEADS * HEAD_DIM), D ** -0.5, 0.09375, ((0, 16), (1, 2))),
        "v_ret": scatter_about(streams_of[7], (D, RET_HEADS * HEAD_DIM), D ** -0.5, 0.09375, ((0, 16), (1, 2))),
        "out_att": scatter_about(streams_of[8], (ATT_HEADS * HEAD_DIM, D), ((ATT_HEADS + RET_HEADS) * HEAD_DIM) ** -0.5, 0.109375, ((0, 2), (1, 16))),
        "out_ret": scatter_about(streams_of[9], (RET_HEADS * HEAD_DIM, D), ((ATT_HEADS + RET_HEADS) * HEAD_DIM) ** -0.5, 0.109375, ((0, 2), (1, 16))),
        "sink": jnp.clip(3.0 + 4.0 * jax.random.uniform(streams_of[10], (ATT_HEADS,), jnp.float32) ** steps_of(streams_of[10], (ATT_HEADS,), ((0, 2),), -0.2, 0.2), 3.0, 7.0),
        "decay_log": draw_decay_log(jax.random.fold_in(streams_of[12], 71), 0),
    }


def rotate(values, angles):
    half = values.shape[-1] // 2
    first = values[..., :half]
    second = values[..., half:]
    cosine = jnp.cos(angles)[:, None, :]
    sine = jnp.sin(angles)[:, None, :]
    return jnp.concatenate([first * cosine - second * sine, second * cosine + first * sine], axis=-1)

def angle_table(positions):
    freqs = 10000.0 ** (-jnp.arange(0, HEAD_DIM, 2).astype(jnp.float32) / HEAD_DIM)
    return positions[:, None] * freqs[None, :]

def window_attention(queries, padded_keys, padded_values, sink_logit, offset, total_rows, block_rows):
    count = queries.shape[0] // block_rows
    nearby_memory = queries.shape[1]
    group = queries.shape[2]

    def single_block(index):
        begin = index * block_rows
        block_query = lax.dynamic_slice_in_dim(queries, begin, block_rows, 0).astype(jnp.float32)
        block_keys = lax.dynamic_slice_in_dim(padded_keys, begin, block_rows + 2 * SPAN_RADIUS, 0).astype(jnp.float32)
        block_values = lax.dynamic_slice_in_dim(padded_values, begin, block_rows + 2 * SPAN_RADIUS, 0).astype(jnp.float32)
        scores = jnp.einsum('qhgd,khd->hgqk', block_query, block_keys) * HEAD_DIM ** (-0.5)
        query_pos = offset + begin + jnp.arange(block_rows, dtype=jnp.int32)
        key_pos = offset + begin - SPAN_RADIUS + jnp.arange(block_rows + 2 * SPAN_RADIUS, dtype=jnp.int32)
        spacing = key_pos[None, :] - query_pos[:, None]
        valid = (jnp.abs(spacing) <= SPAN_RADIUS) & (key_pos >= 0)[None, :] & (key_pos < total_rows)[None, :]
        masked = jnp.where(valid, scores, -jnp.inf)
        top = jnp.maximum(lax.optimization_barrier(jnp.max(masked, axis=-1)), sink_logit[:, :, None])
        expo = jnp.exp(masked - top[..., None])
        total = lax.optimization_barrier(jnp.sum(expo, axis=-1)) + jnp.exp(sink_logit[:, :, None] - top)
        logs = top + jnp.log(total)
        probs = (expo / total[..., None]).astype(jnp.bfloat16)
        result = jnp.einsum('hgqk,khd->qhgd', probs.astype(jnp.float32), block_values).astype(jnp.bfloat16)
        return (result.reshape(block_rows, nearby_memory * group * HEAD_DIM), logs.reshape(nearby_memory * group, block_rows))
    outs, logs = lax.map(single_block, jnp.arange(count, dtype=jnp.int32))
    return (outs.reshape(queries.shape[0], -1), jnp.moveaxis(logs, 0, 1).reshape(logs.shape[1], -1))

def retention(queries, keys, values, decay):
    blocks = queries.shape[0] // TOK_DEV
    heads = queries.shape[1]
    highest = lax.Precision.HIGHEST
    query_b = queries.reshape(blocks, TOK_DEV, heads, HEAD_DIM)
    key_b = keys.reshape(blocks, TOK_DEV, heads, HEAD_DIM)
    value_b = values.reshape(blocks, TOK_DEV, heads, HEAD_DIM)
    decay_b = jnp.moveaxis(decay.reshape(heads, blocks, TOK_DEV), 1, 0)

    def local(items):
        query_f = items[0].astype(jnp.float32)
        key_f = items[1].astype(jnp.float32)
        value_f = items[2].astype(jnp.float32)
        cumul = jnp.cumsum(items[3], axis=1)
        last = cumul[:, -1]
        scores = jnp.einsum('qhd,khd->hqk', query_f, key_f)
        weights = jnp.exp(-jnp.abs(cumul[:, :, None] - cumul[:, None, :]))
        inner = jnp.einsum('hqk,khd->qhd', scores * weights, value_f, precision=highest)
        forward = jnp.einsum('hk,khd,khe->hde', jnp.exp(last[:, None] - cumul), key_f, value_f, precision=highest)
        backward = jnp.einsum('hk,khd,khe->hde', jnp.exp(cumul), key_f, value_f, precision=highest)
        return (inner, forward, backward, jnp.exp(last), cumul)
    inner, forward, backward, totals, cumuls = lax.map(local, (query_b, key_b, value_b, decay_b))

    def step(carry, item):
        return (item[0][:, None, None] * carry + item[1], carry)
    zero = jnp.zeros(forward.shape[1:], jnp.float32)
    _, before = lax.scan(step, zero, (totals, forward))
    _, after = lax.scan(step, zero, (totals, backward), reverse=True)
    query_f = query_b.astype(jnp.float32)
    lead = jnp.moveaxis(jnp.exp(cumuls), 1, 2)[..., None]
    trail = jnp.moveaxis(jnp.exp(cumuls[:, :, -1:] - cumuls), 1, 2)[..., None]
    carried = lead * jnp.einsum('bqhd,bhde->bqhe', query_f, before, precision=highest)
    carried = carried + trail * jnp.einsum('bqhd,bhde->bqhe', query_f, after, precision=highest)
    blended_output = inner + carried
    middle_point = blended_output - lax.optimization_barrier(jnp.mean(blended_output, axis=-1, keepdims=True))
    normed = middle_point * lax.rsqrt(lax.optimization_barrier(jnp.mean(middle_point * middle_point, axis=-1, keepdims=True)) + 1e-06)
    return normed.astype(jnp.bfloat16).reshape(queries.shape[0], heads * HEAD_DIM)

def reference(tokens, gain, q_att, k_att, v_att, q_ret, k_ret, v_ret, out_att, out_ret, sink, decay_log):
    widened = tokens.astype(jnp.float32)
    inverse = lax.rsqrt(lax.optimization_barrier(jnp.sum(widened * widened, axis=1)) / D + 1e-06)[:, None]
    scaled = (widened * gain).astype(jnp.bfloat16)

    def project(weight):
        return jnp.dot(scaled, weight, preferred_element_type=jnp.float32) * inverse
    angles = angle_table(jnp.arange(TOKENS).astype(jnp.float32))
    group = ATT_HEADS // KV_HEADS
    att_query = rotate(project(q_att).reshape(TOKENS, ATT_HEADS, HEAD_DIM), angles).astype(jnp.bfloat16)
    att_key = rotate(project(k_att).reshape(TOKENS, KV_HEADS, HEAD_DIM), angles).astype(jnp.bfloat16)
    att_value = project(v_att).astype(jnp.bfloat16).reshape(TOKENS, KV_HEADS, HEAD_DIM)
    padding = ((SPAN_RADIUS, SPAN_RADIUS), (0, 0), (0, 0))
    att_out, log_weight = window_attention(att_query.reshape(TOKENS, KV_HEADS, group, HEAD_DIM), jnp.pad(att_key, padding), jnp.pad(att_value, padding), sink.reshape(KV_HEADS, group), 0, TOKENS, min(TOK_DEV, 512))
    ret_query = project(q_ret).astype(jnp.bfloat16).reshape(TOKENS, RET_HEADS, HEAD_DIM)
    ret_key = (jnp.dot(scaled, k_ret, preferred_element_type=jnp.float32) * (inverse * HEAD_DIM ** (-0.5))).astype(jnp.bfloat16).reshape(TOKENS, RET_HEADS, HEAD_DIM)
    ret_value = project(v_ret).astype(jnp.bfloat16).reshape(TOKENS, RET_HEADS, HEAD_DIM)
    ret_out = retention(ret_query, ret_key, ret_value, decay_log)
    att_width = ATT_HEADS * HEAD_DIM // N_TP
    ret_width = RET_HEADS * HEAD_DIM // N_TP
    summed = jnp.zeros((TOKENS, D), jnp.float32)
    for member in range(N_TP):
        term = jnp.dot(att_out[:, member * att_width:(member + 1) * att_width], out_att[member * att_width:(member + 1) * att_width], preferred_element_type=jnp.float32)
        term = term + jnp.dot(ret_out[:, member * ret_width:(member + 1) * ret_width], out_ret[member * ret_width:(member + 1) * ret_width], preferred_element_type=jnp.float32)
        summed = summed + lax.optimization_barrier(term.astype(jnp.bfloat16)).astype(jnp.float32)
    return (summed.astype(jnp.bfloat16), log_weight)
```

```python
import functools

import jax
import jax.numpy as jnp
from jax import lax
from jax.experimental import pallas as pl
from jax.experimental.pallas import tpu as pltpu
from jax.sharding import Mesh, PartitionSpec as P

D = 4096
HEAD_DIM = 128
SPAN_RADIUS = 128
CHUNK = 256


def with_halo(shard, sides, width):
    for axis, dim in sides:
        peers, length = (lax.axis_size(axis), shard.shape[dim])
        up = [(i, (i + 1) % peers) for i in range(peers - 1)]
        down = [(j, i) for i, j in up]
        last = lax.slice_in_dim(shard, length - width, length, axis=dim)
        initial = lax.slice_in_dim(shard, 0, width, axis=dim)
        before = lax.ppermute(last, axis, up)
        after = lax.ppermute(initial, axis, down)
        shard = jnp.concatenate([before, shard, after], axis=dim)
    return shard


def entering(shard, axis, combine, identity, reverse):
    peers, index = (lax.axis_size(axis), lax.axis_index(axis))
    everything = jax.tree.map(
        lambda part, kind: lax.all_gather(part.astype(kind), axis),
        shard,
        (jnp.bfloat16, jnp.bfloat16),
    )
    start = jax.tree.map(
        lambda part, zero: jnp.broadcast_to(jnp.asarray(zero, part.dtype), part.shape),
        shard,
        identity,
    )

    def turn(k, before):
        at = peers - 1 - k if reverse else k
        reached = at > index if reverse else at < index
        new = combine(
            before, jax.tree.map(lambda part, own: part[at].astype(own.dtype), everything, shard)
        )
        return jax.tree.map(lambda a, b: jnp.where(reached, a, b), new, before)

    return lax.fori_loop(0, peers, turn, start)


def rotate(values, angles):
    half = values.shape[-1] // 2
    first = values[..., :half]
    second = values[..., half:]
    cosine = jnp.cos(angles)[:, None, :]
    sine = jnp.sin(angles)[:, None, :]
    return jnp.concatenate(
        [first * cosine - second * sine, second * cosine + first * sine], axis=-1
    )


def fold_with(weights, piece):
    return tuple((jnp.dot(piece, weight, preferred_element_type=jnp.float32) for weight in weights))


def chain(earlier, later):
    return (earlier[0] * later[0], later[0][:, None, None] * earlier[1] + later[1])


def shards(
    tokens, gain, q_att, k_att, v_att, q_ret, k_ret, v_ret, out_att, out_ret, sink, decay_log
):
    tok_rows = tokens.shape[0]
    att_local = sink.shape[0]
    nearby_memory = k_att.shape[1] // HEAD_DIM
    ret_local = q_ret.shape[1] // HEAD_DIM
    group = att_local // nearby_memory
    total_rows = tok_rows * lax.axis_size("sp")
    offset = lax.axis_index("sp") * tok_rows
    highest = lax.Precision.HIGHEST
    widened = tokens.astype(jnp.float32)
    squares = lax.psum(jnp.sum(widened * widened, axis=1), "tp")
    inverse = lax.rsqrt(squares / D + 1e-06)[:, None]
    scaled = (widened * gain).astype(jnp.bfloat16)
    wide_qa, wide_ka, wide_va, wide_qr, wide_kr, wide_vr = (
        lax.all_gather(q_att, "sp", axis=0, tiled=True),
        lax.all_gather(k_att, "sp", axis=0, tiled=True),
        lax.all_gather(v_att, "sp", axis=0, tiled=True),
        lax.all_gather(q_ret, "sp", axis=0, tiled=True),
        lax.all_gather(k_ret, "sp", axis=0, tiled=True),
        lax.all_gather(v_ret, "sp", axis=0, tiled=True),
    )
    every_weight = (wide_qa, wide_ka, wide_va, wide_qr, wide_kr, wide_vr)
    proj_qa, proj_ka, proj_va, proj_qr, proj_kr, proj_vr = fold_with(
        every_weight, lax.all_gather(scaled, "tp", axis=1, tiled=True)
    )
    positions = (offset + jnp.arange(tok_rows, dtype=jnp.int32)).astype(jnp.float32)
    freqs = 10000.0 ** (-jnp.arange(0, HEAD_DIM, 2).astype(jnp.float32) / HEAD_DIM)
    angles = positions[:, None] * freqs[None, :]
    att_query = rotate((proj_qa * inverse).reshape(tok_rows, att_local, HEAD_DIM), angles).astype(
        jnp.bfloat16
    )
    att_key = rotate((proj_ka * inverse).reshape(tok_rows, nearby_memory, HEAD_DIM), angles).astype(
        jnp.bfloat16
    )
    att_value = (proj_va * inverse).astype(jnp.bfloat16).reshape(tok_rows, nearby_memory, HEAD_DIM)
    stacked = jnp.stack([att_key, att_value])
    widened_pair = with_halo(stacked, (("sp", 1),), SPAN_RADIUS)
    block_rows = min(tok_rows, 512)
    sink_logit = sink.reshape(nearby_memory, group)
    grouped_query = att_query.reshape(tok_rows, nearby_memory, group, HEAD_DIM)

    def attend_block(index):
        begin = index * block_rows
        block_keys = widened_pair[0]
        block_values = widened_pair[1]
        scores = jnp.einsum(
            "qhgd,khd->hgqk", grouped_query, block_keys, preferred_element_type=jnp.float32
        ) * HEAD_DIM ** (-0.5)
        query_pos = offset + begin + jnp.arange(block_rows, dtype=jnp.int32)
        key_pos = (
            offset + begin - SPAN_RADIUS + jnp.arange(block_rows + 2 * SPAN_RADIUS, dtype=jnp.int32)
        )
        spacing = key_pos[None, :] - query_pos[:, None]
        valid = (
            (jnp.abs(spacing) <= SPAN_RADIUS)
            & (key_pos >= 0)[None, :]
            & (key_pos < total_rows)[None, :]
        )
        masked = jnp.where(valid, scores, -jnp.inf)
        top = jnp.maximum(jnp.max(masked, axis=-1), sink_logit[:, :, None])
        expo = jnp.exp(masked - top[..., None])
        total = jnp.sum(expo, axis=-1) + jnp.exp(sink_logit[:, :, None] - top)
        logs = top + jnp.log(total)
        probs = (expo / total[..., None]).astype(jnp.bfloat16)
        result = jnp.einsum(
            "hgqk,khd->qhgd", probs, block_values, preferred_element_type=jnp.float32
        ).astype(jnp.bfloat16)
        return (
            result.reshape(block_rows, att_local * HEAD_DIM),
            logs.reshape(att_local, block_rows),
        )

    att_blocks, log_blocks = lax.map(
        attend_block, jnp.arange(tok_rows // block_rows, dtype=jnp.int32)
    )
    att_out = att_blocks.reshape(tok_rows, att_local * HEAD_DIM)
    log_weight = jnp.moveaxis(log_blocks, 0, 1).reshape(att_local, tok_rows)
    ret_query = (proj_qr * inverse).astype(jnp.bfloat16).reshape(tok_rows, ret_local, HEAD_DIM)
    ret_key = (
        (proj_kr * (inverse * HEAD_DIM ** (-0.5)))
        .astype(jnp.bfloat16)
        .reshape(tok_rows, ret_local, HEAD_DIM)
    )
    ret_value = (proj_vr * inverse).astype(jnp.bfloat16).reshape(tok_rows, ret_local, HEAD_DIM)
    cumul = jnp.cumsum(decay_log, axis=1)
    last = cumul[:, -1]
    query_f = ret_query.astype(jnp.float32)
    key_f = ret_key.astype(jnp.float32)
    value_f = ret_value.astype(jnp.float32)
    ret_scores = jnp.einsum("qhd,khd->hqk", ret_query, ret_key, preferred_element_type=jnp.float32)
    decay_weights = jnp.exp(-jnp.abs(cumul[:, :, None] - cumul[:, None, :]))
    inner = jnp.einsum("hqk,khd->qhd", ret_scores * decay_weights, value_f, precision=highest)
    trailing = jnp.exp(last[:, None] - cumul)
    leading = jnp.exp(cumul)
    forward_state = jnp.einsum("hk,khd,khe->hde", trailing, key_f, value_f, precision=highest)
    backward_state = jnp.einsum("hk,khd,khe->hde", leading, key_f, value_f, precision=highest)
    decay_total = jnp.exp(last)
    identity = (jnp.ones_like(decay_total), jnp.zeros_like(forward_state))
    from_before = entering((decay_total, forward_state), "sp", chain, identity, False)[1]
    from_after = entering((decay_total, backward_state), "sp", chain, identity, True)[1]
    carried = leading.T[:, :, None] * jnp.einsum(
        "qhd,hde->qhe", query_f, from_before, precision=highest
    )
    carried = carried + trailing.T[:, :, None] * jnp.einsum(
        "qhd,hde->qhe", query_f, from_after, precision=highest
    )
    blended_output = inner + carried
    middle_point = blended_output - jnp.mean(blended_output, axis=-1, keepdims=True)
    normed = middle_point * lax.rsqrt(
        jnp.mean(middle_point * middle_point, axis=-1, keepdims=True) + 1e-06
    )
    ret_out = normed.astype(jnp.bfloat16).reshape(tok_rows, ret_local * HEAD_DIM)
    wide_out_att, wide_out_ret = (
        lax.all_gather(out_att, "sp", axis=1, tiled=True),
        lax.all_gather(out_ret, "sp", axis=1, tiled=True),
    )
    mixed = lax.psum_scatter(
        (
            jnp.dot(att_out, wide_out_att, preferred_element_type=jnp.float32)
            + jnp.dot(ret_out, wide_out_ret, preferred_element_type=jnp.float32)
        ).astype(jnp.bfloat16),
        "tp",
        scatter_dimension=0,
        tiled=True,
    )
    return (mixed, log_weight)


F32 = jnp.float32
BF16 = jnp.bfloat16
HIGHEST = lax.Precision.HIGHEST
MEMBERS = 4
PLANES = 4
HALVES = 2
Z, ME, CORE, SLOT = 0, 1, 2, 3
ANY = pl.BlockSpec(memory_space=pl.ANY)
SMEM = pl.BlockSpec(memory_space=pltpu.SMEM)
VMEM = pl.BlockSpec(memory_space=pltpu.VMEM)


def swap(value, axis, k=1):
    return lax.ppermute(value, axis, [(i, i ^ k) for i in range(lax.axis_size(axis))])


def at(value, unit):
    return pl.multiple_of(value * unit, unit)


class Copies:
    def __init__(self, sems):
        self.sems, self.made = sems, []

    def start(self, source, target, when=None):
        copy = pltpu.make_async_copy(source, target, self.sems.at[len(self.made)])
        if when is None:
            copy.start()
        else:
            pl.when(when)(copy.start)
        self.made.append(copy)

    def choose(self, options, target):
        sem = self.sems.at[len(self.made)]
        for when, source in options:
            pl.when(when)(pltpu.make_async_copy(source, target, sem).start)
        self.made.append(pltpu.make_async_copy(options[0][1], target, sem))

    def wait(self, first=0, last=None):
        for copy in self.made[first:last]:
            copy.wait()


def call(body, name, out, ins, scratch, flops=0):
    return pl.pallas_call(
        body,
        name=name,
        out_shape=[jax.ShapeDtypeStruct(shape, kind) for shape, kind, _ in out],
        in_specs=ins,
        out_specs=[spec for _, _, spec in out],
        scratch_shapes=scratch,
        cost_estimate=pl.CostEstimate(flops=flops, bytes_accessed=1 << 20, transcendentals=0),
    )


def pack_body(ids, qa, ka, va, qr, kr, vr, *refs):
    att, ret, sems = refs[:MEMBERS], refs[MEMBERS:-1], refs[-1]
    copies = Copies(sems)
    for k in range(MEMBERS):
        member = ids[ME] ^ k
        for target, sources in ((att[k], (qa, ka, va)), (ret[k], (qr, kr, vr))):
            done = 0
            for source in sources:
                width = source.shape[1] // MEMBERS
                copies.start(
                    source.at[:, pl.ds(at(member, width), width)],
                    target.at[:, done : done + width],
                )
                done += width
    copies.wait()


def pack(ids, weights):
    rows = weights[0].shape[0]
    widths = [sum(w.shape[1] for w in part) // MEMBERS for part in (weights[:3], weights[3:])]
    out = [((rows, w), BF16, VMEM) for w in widths for _ in range(MEMBERS)]
    sems = [pltpu.SemaphoreType.DMA((6 * MEMBERS,))]
    got = call(pack_body, "pack", out, [SMEM] + [ANY] * 6, sems)(ids, *weights)
    return got[:MEMBERS], got[MEMBERS:]


def plane_pieces(value):
    half = value.shape[0] // 2
    one = swap(value, "si", 1)
    two = swap(value, "si", 2)
    return [value, one, two, swap(one[:half], "si", 2), swap(two[half:], "si", 1)]


def piece_rows(k, rows):
    half = rows // 2
    return ((0, 0, rows), (1, 0, rows), (2, 0, rows), (3, 0, half), (3, half, half))[k]


def load_tokens(copies, ids, target, base, near, far):
    rows, feats = near[0].shape
    for k in range(5):
        other, start, size = piece_rows(k, rows)
        row = pl.multiple_of(base + at(ids[ME] ^ other, rows) + start, size)
        for core, source in ((ids[CORE], near[k]), (1 - ids[CORE], far[k])):
            copies.start(
                source, target.at[pl.ds(row, size), pl.ds(at(core, feats), feats)]
            )


def load_chunk(copies, ids, target, plane, options):
    rows = options[0][1].shape[0] // MEMBERS
    for k in range(MEMBERS):
        start = at(plane * MEMBERS + (ids[ME] ^ k), rows)
        copies.choose(
            [(when, source.at[k * rows : (k + 1) * rows]) for when, source in options],
            target.at[pl.ds(start, rows)],
        )


def line_options(ids, up, down):
    z = ids[Z]
    return (
        [(z == 0, down[1]), (z != 0, up[1])],
        [(z == 0, down[2]), ((z == 1) | (z == 2), down[1]), (z == 3, up[2])],
        [(z == 0, down[3]), (z == 1, down[2]), (z == 2, up[2]), (z == 3, up[3])],
    )


def line(value):
    up, down = [value], [value]
    for s in range(1, PLANES):
        up.append(lax.ppermute(up[-1], "so", [(i, i + 1) for i in range(s - 1, PLANES - 1)]))
        down.append(lax.ppermute(down[-1], "so", [(i + 1, i) for i in range(PLANES - s)]))
    return up[1:] + down[1:]


def turn(value, cosine, sine):
    return value * cosine + pltpu.roll(value, HEAD_DIM // 2, 1) * sine


def att_proj_body(ids, inverse, cosine, sine, *refs):
    near, far, own = refs[:5], refs[5:10], refs[10]
    up, down = (None,) + refs[11:14], (None,) + refs[14:17]
    query, pair, tokens, weights, sems = refs[17:]
    copies = Copies(sems)
    load_tokens(copies, ids, tokens, 0, near, far)
    always = ids[Z] >= 0
    load_chunk(copies, ids, weights, ids[Z], [(always, own)])
    for slot, options in enumerate(line_options(ids, up, down)):
        load_chunk(copies, ids, weights, ids[SLOT + slot], options)
    copies.wait()
    width = query.shape[1]
    for start in range(0, query.shape[0], CHUNK):
        part = slice(start, start + CHUNK)
        got = jnp.dot(tokens[part], weights[...], preferred_element_type=F32) * inverse[part]
        for g in range(0, width, HEAD_DIM):
            head = slice(g, g + HEAD_DIM)
            query[part, head] = turn(got[:, head], cosine[part], sine[part]).astype(BF16)
        key = got[:, width : width + HEAD_DIM]
        pair[0, part] = turn(key, cosine[part], sine[part]).astype(BF16)
        pair[1, part] = got[:, width + HEAD_DIM :].astype(BF16)


def att_proj(ids, inverse, cosine, sine, near, far, own, others):
    rows = inverse.shape[0]
    width = own.shape[1]
    return call(
        att_proj_body,
        "att_proj",
        [((rows, width - 2 * HEAD_DIM), BF16, VMEM), ((2, rows, HEAD_DIM), BF16, VMEM)],
        [SMEM] + [VMEM] * 3 + [ANY] * 17,
        [
            pltpu.VMEM((rows, D), BF16),
            pltpu.VMEM((D, width), BF16),
            pltpu.SemaphoreType.DMA((10 + MEMBERS * PLANES,)),
        ],
        2 * rows * D * width,
    )(ids, inverse, cosine, sine, *near, *far, own, *others)


def attend_body(ids, sink, query, pair, before, after, out, logs, keys, values, *, total_rows):
    rows, width = query.shape
    for target, part in ((keys, 0), (values, 1)):
        target[:SPAN_RADIUS] = before[part]
        target[SPAN_RADIUS : SPAN_RADIUS + rows] = pair[part]
        target[SPAN_RADIUS + rows :] = after[part]
    wide = CHUNK + 2 * SPAN_RADIUS
    row = lax.broadcasted_iota(jnp.int32, (CHUNK, wide), 0)
    column = lax.broadcasted_iota(jnp.int32, (CHUNK, wide), 1)
    near = jnp.abs(column - SPAN_RADIUS - row) <= SPAN_RADIUS
    for start in range(0, rows, CHUNK):
        key_pos = ids[Z] * rows + start - SPAN_RADIUS + column
        valid = near & (key_pos >= 0) & (key_pos < total_rows)
        for g in range(width // HEAD_DIM):
            head = slice(g * HEAD_DIM, (g + 1) * HEAD_DIM)
            scores = lax.dot_general(
                query[start : start + CHUNK, head],
                keys[start : start + wide],
                (((1,), (1,)), ((), ())),
                preferred_element_type=F32,
            ) * HEAD_DIM ** (-0.5)
            masked = jnp.where(valid, scores, -jnp.inf)
            limit = sink[ids[ME] * (width // HEAD_DIM) + g]
            top = jnp.maximum(jnp.max(masked, axis=1, keepdims=True), limit)
            expo = jnp.exp(masked - top)
            total = jnp.sum(expo, axis=1, keepdims=True) + jnp.exp(limit - top)
            logs[start : start + CHUNK, g : g + 1] = top + jnp.log(total)
            probs = (expo / total).astype(BF16)
            out[start : start + CHUNK, head] = jnp.dot(
                probs, values[start : start + wide], preferred_element_type=F32
            ).astype(BF16)


def attend(ids, sink, query, pair, before, after):
    rows, width = query.shape
    padded = pltpu.VMEM((rows + 2 * SPAN_RADIUS, HEAD_DIM), BF16)
    return call(
        functools.partial(attend_body, total_rows=rows * PLANES),
        "attend",
        [((rows, width), BF16, VMEM), ((rows, width // HEAD_DIM), F32, VMEM)],
        [SMEM, SMEM] + [VMEM] * 4,
        [padded, padded],
        8 * rows * width * CHUNK,
    )(ids, sink, query, pair, before, after)


def exact_dot(a, b, contract):
    return lax.dot_general(
        a, b, (contract, ((), ())), precision=HIGHEST, preferred_element_type=F32
    )


def ret_proj_body(ids, inverse, cumul, *refs):
    sets, own, hops = (refs[:10], refs[10:20]), refs[20], refs[21:24]
    query, key, value, states, parcel, tokens, weights, sems = refs[24:]
    rows = query.shape[0]
    middle = (ids[Z] == 1) | (ids[Z] == 2)

    @pl.when(middle)
    def _():
        copies = Copies(sems)
        always = ids[Z] >= 0
        for k, (hop, other) in enumerate(zip((own,) + hops, (0, 1, 3, 2))):
            load_chunk(copies, ids, weights, ids[Z] ^ other, [(always, hop)])
        first = jnp.where(ids[Z] == 1, rows // 2, 0)
        for base, pieces in zip((first, rows // 2 - first), sets):
            load_tokens(copies, ids, tokens, base, pieces[:5], pieces[5:])
        copies.wait()
        count = rows // CHUNK
        for b in range(count):
            part = slice(b * CHUNK, (b + 1) * CHUNK)
            got = jnp.dot(tokens[part], weights[...], preferred_element_type=F32)
            scale = inverse[part]
            query[part] = (got[:, :HEAD_DIM] * scale).astype(BF16)
            k = (got[:, HEAD_DIM : 2 * HEAD_DIM] * (scale * HEAD_DIM ** (-0.5))).astype(BF16)
            v = (got[:, 2 * HEAD_DIM :] * scale).astype(BF16)
            key[part] = k
            value[part] = v
            along = cumul[part]
            last = along[CHUNK - 1 :]
            kf, vf = k.astype(F32), v.astype(F32)
            states[b] = exact_dot(kf, jnp.exp(last - along) * vf, ((0,), (0,)))
            states[count + b] = exact_dot(kf, jnp.exp(along) * vf, ((0,), (0,)))
        ahead, behind = jnp.zeros((HEAD_DIM, HEAD_DIM), F32), jnp.zeros((HEAD_DIM, HEAD_DIM), F32)
        for b in range(count):
            r = count - 1 - b
            fade = jnp.exp(cumul[(b + 1) * CHUNK - 1 : (b + 1) * CHUNK])
            ahead = fade * ahead + states[b]
            fade = jnp.exp(cumul[(r + 1) * CHUNK - 1 : (r + 1) * CHUNK])
            behind = fade * behind + states[count + r]
        parcel[...] = jnp.where(ids[Z] == 1, ahead, behind)

    @pl.when(jnp.logical_not(middle))
    def _():
        parcel[...] = jnp.zeros_like(parcel)


def ret_proj(ids, inverse, cumul, near, far, next_near, next_far, own, hops):
    rows = inverse.shape[0]
    width = own.shape[1]
    square = (HEAD_DIM, HEAD_DIM)
    return call(
        ret_proj_body,
        "ret_proj",
        [((rows, HEAD_DIM), BF16, VMEM)] * 3
        + [((2 * rows // CHUNK,) + square, F32, VMEM), (square, F32, VMEM)],
        [SMEM] + [VMEM] * 2 + [ANY] * 24,
        [
            pltpu.VMEM((rows, D), BF16),
            pltpu.VMEM((D, width), BF16),
            pltpu.SemaphoreType.DMA((20 + MEMBERS * PLANES,)),
        ],
        2 * rows * D * width,
    )(ids, inverse, cumul, *near, *far, *next_near, *next_far, own, *hops)


def retain_body(ids, query, key, value, cumul, cumul_row, states, parcel, out, afters):
    rows = query.shape[0]
    count = rows // CHUNK
    middle = (ids[Z] == 1) | (ids[Z] == 2)

    @pl.when(middle)
    def _():
        after = jnp.where(ids[Z] == 1, parcel[...], 0.0)
        for r in reversed(range(count)):
            afters[r] = after
            fade = jnp.exp(cumul[(r + 1) * CHUNK - 1 : (r + 1) * CHUNK])
            after = fade * after + states[count + r]
        before = jnp.where(ids[Z] == 2, parcel[...], 0.0)
        for b in range(count):
            part = slice(b * CHUNK, (b + 1) * CHUNK)
            q, k, v = query[part], key[part], value[part]
            along = cumul[part]
            last = along[CHUNK - 1 :]
            scores = lax.dot_general(
                q, k, (((1,), (1,)), ((), ())), preferred_element_type=F32
            )
            decay = jnp.exp(-jnp.abs(along - cumul_row[b : b + 1]))
            qf, vf = q.astype(F32), v.astype(F32)
            mix = exact_dot(scores * decay, vf, ((1,), (0,)))
            mix = mix + jnp.exp(along) * exact_dot(qf, before, ((1,), (0,)))
            mix = mix + jnp.exp(last - along) * exact_dot(qf, afters[b], ((1,), (0,)))
            middle_point = mix - jnp.mean(mix, axis=1, keepdims=True)
            spread = jnp.mean(middle_point * middle_point, axis=1, keepdims=True)
            normed = (middle_point * lax.rsqrt(spread + 1e-06)).astype(BF16)
            half = (2 * b) // count
            index = jnp.where(ids[Z] == 1, 1 - half, half)
            start = b * CHUNK - half * (rows // 2)
            out[index, start : start + CHUNK] = normed
            before = jnp.exp(last) * before + states[b]

    @pl.when(jnp.logical_not(middle))
    def _():
        out[...] = jnp.zeros_like(out)


def retain(ids, query, key, value, cumul, cumul_row, states, parcel):
    rows = query.shape[0]
    return call(
        retain_body,
        "retain",
        [((2, rows // 2, HEAD_DIM), BF16, VMEM)],
        [SMEM] + [VMEM] * 7,
        [pltpu.VMEM((rows // CHUNK, HEAD_DIM, HEAD_DIM), F32)],
        8 * rows * HEAD_DIM * CHUNK,
    )(ids, query, key, value, cumul, cumul_row, states, parcel)[0]


def out_proj_body(ids, *refs, slots):
    att, ret, own = refs[:5], refs[5:9], refs[9]
    up, down = (None,) + refs[10:13], (None,) + refs[13:16]
    parts, hidden, weights, sems = refs[16:]
    copies = Copies(sems)
    rows, att_width = att[0].shape
    ret_width = ret[0].shape[1]
    for k in range(5):
        other, start, size = piece_rows(k, rows)
        column = at(ids[ME] ^ other, att_width)
        copies.start(att[k], hidden.at[start : start + size, pl.ds(column, att_width)])
    for k in range(MEMBERS):
        column = MEMBERS * att_width + (ids[ME] ^ k) * ret_width
        column = pl.multiple_of(column, ret_width)
        copies.start(ret[k], hidden.at[:, pl.ds(column, ret_width)])
    options = ([(ids[Z] >= 0, own)],) + line_options(ids, up, down)
    for n, slot in enumerate(slots):
        copies.choose(options[slot], weights.at[n])
    copies.wait()
    own_rows = rows // MEMBERS // HALVES
    for n in range(len(slots)):
        for member in range(MEMBERS):
            start = member * HALVES * own_rows
            got = jnp.dot(
                hidden[start : start + HALVES * own_rows],
                weights[n],
                preferred_element_type=F32,
            ).astype(BF16)
            for half in range(HALVES):
                parts[half ^ ids[CORE], n, member] = got[half * own_rows : (half + 1) * own_rows]


def out_proj(ids, att, ret, own, others, slots):
    rows = att[0].shape[0]
    depth, width = own.shape
    return call(
        functools.partial(out_proj_body, slots=slots),
        "out_proj%d" % len(slots),
        [((HALVES, len(slots), MEMBERS, rows // MEMBERS // HALVES, width), BF16, VMEM)],
        [SMEM] + [ANY] * 16,
        [
            pltpu.VMEM((rows, depth), BF16),
            pltpu.VMEM((len(slots), depth, width), BF16),
            pltpu.SemaphoreType.DMA((9 + len(slots),)),
        ],
        2 * rows * depth * width * len(slots),
    )(ids, *att, *ret, own, *others)[0]


def place_body(ids, *refs, counts):
    parts, mixed, sems = refs[:-2], refs[-2], refs[-1]
    copies = Copies(sems)
    width = parts[0].shape[2]
    slot = 0
    for n, count in enumerate(counts):
        for i in range(count):
            plane = ids[Z] if slot == 0 else ids[SLOT + slot - 1]
            for k in range(MEMBERS):
                column = at(plane * MEMBERS + (ids[ME] ^ k), width)
                copies.start(parts[n * MEMBERS + k].at[i], mixed.at[:, pl.ds(column, width)])
            slot += 1
    copies.wait()


def place(ids, groups):
    parts = [part for group in groups for part in group]
    counts = [group[0].shape[0] for group in groups]
    rows, width = parts[0].shape[1:]
    return call(
        functools.partial(place_body, counts=counts),
        "place",
        [((rows, width * MEMBERS * PLANES), BF16, VMEM)],
        [SMEM] + [ANY] * len(parts),
        [pltpu.SemaphoreType.DMA((MEMBERS * PLANES,))],
    )(ids, *parts)[0]


def pick(value, index, axis=0):
    return lax.dynamic_index_in_dim(value, index, axis, keepdims=False)


def plane_shards(
    tokens, gain, q_att, k_att, v_att, q_ret, k_ret, v_ret, out_att, out_ret, sink, decay_log
):
    tok_rows = tokens.shape[0]
    me, z, core = lax.axis_index("si"), lax.axis_index("so"), lax.axis_index("tp")
    heads = sink.shape[0]
    group = heads // MEMBERS
    rows = tok_rows * MEMBERS
    slot_table = jnp.array([[1, 2, 3], [0, 2, 3], [1, 3, 0], [2, 1, 0]], jnp.int32)
    ids = jnp.concatenate([jnp.stack([z, me, core]).astype(jnp.int32), pick(slot_table, z)])
    inward = [(0, 1), (3, 2)]
    across = [(1, 2), (2, 1)]

    att_sub, ret_sub = pack(ids, (q_att, k_att, v_att, q_ret, k_ret, v_ret))
    widened = tokens.astype(F32)
    scaled = (widened * gain).astype(BF16)
    att_own = jnp.concatenate(
        [att_sub[0]] + [swap(att_sub[k], "si", k) for k in range(1, MEMBERS)], axis=0
    )
    near = plane_pieces(scaled)
    ret_own = jnp.concatenate(
        [ret_sub[0]] + [swap(ret_sub[k], "si", k) for k in range(1, MEMBERS)], axis=0
    )
    far = [swap(piece, "tp") for piece in near]
    att_line = line(att_own)
    hop_0 = lax.ppermute(ret_own, "so", inward)
    hop_1 = lax.ppermute(ret_own, "so", across)
    hop_2 = lax.ppermute(hop_0, "so", across)
    next_own = lax.ppermute(scaled, "so", inward)
    next_near = [
        next_own,
        swap(next_own, "si", 1),
        swap(next_own, "si", 2),
        lax.ppermute(near[3], "so", inward),
        lax.ppermute(near[4], "so", inward),
    ]
    next_far = [swap(piece, "tp") for piece in next_near]
    out_own = jnp.concatenate([out_att, out_ret], axis=0)
    out_line = line(out_own)

    squares = lax.psum(jnp.sum(widened * widened, axis=1), "tp")
    inverse = lax.rsqrt(squares / D + 1e-06)
    mine = jnp.zeros((2, MEMBERS, tok_rows), F32)
    for k in range(MEMBERS):
        piece = jnp.stack([inverse, pick(decay_log, me ^ k)])
        piece = piece if k == 0 else swap(piece, "si", k)
        mine = lax.dynamic_update_index_in_dim(mine, piece, me ^ k, 1)
    mine = mine.reshape(2, rows)
    nearby = lax.ppermute(mine, "so", inward)
    pair_rows = jnp.where(z == 1, jnp.stack([nearby, mine]), jnp.stack([mine, nearby]))
    pair_rows = jnp.moveaxis(pair_rows, 1, 0).reshape(2, 2 * rows)
    cumul_row = jnp.cumsum(pair_rows[1].reshape(-1, CHUNK), axis=1)
    cumul = cumul_row.reshape(-1, 1)
    positions = (z * rows + jnp.arange(rows, dtype=jnp.int32)).astype(F32)
    freqs = 10000.0 ** (-jnp.arange(0, HEAD_DIM, 2).astype(F32) / HEAD_DIM)
    angles = positions[:, None] * freqs[None, :]
    cosine, sine = jnp.cos(angles), jnp.sin(angles)
    cosine = jnp.concatenate([cosine, cosine], axis=1)
    sine = jnp.concatenate([-sine, sine], axis=1)

    query, pair = att_proj(
        ids, mine[0][:, None], cosine, sine, near, far, att_own, att_line
    )
    before = lax.ppermute(
        pair[:, rows - SPAN_RADIUS :], "so", [(i, i + 1) for i in range(PLANES - 1)]
    )
    after = lax.ppermute(pair[:, :SPAN_RADIUS], "so", [(i + 1, i) for i in range(PLANES - 1)])
    ret_query, ret_key, ret_value, states, parcel = ret_proj(
        ids, pair_rows[0][:, None], cumul, near, far, next_near, next_far, ret_own,
        (hop_0, hop_1, hop_2),
    )
    parcel = lax.ppermute(parcel, "so", across)
    att_out, logs = attend(ids, sink, query, pair, before, after)
    att_pieces = plane_pieces(att_out)
    ret_out = retain(ids, ret_query, ret_key, ret_value, cumul, cumul_row, states, parcel)
    back = lax.ppermute(ret_out[1], "so", [(1, 0), (2, 3)])
    ret_mine = jnp.where((z == 1) | (z == 2), ret_out[0], back)
    ret_pieces = [ret_mine] + [swap(ret_mine, "si", k) for k in range(1, MEMBERS)]

    groups = []
    for slots in ((0, 1, 2), (3,)):
        parts = out_proj(ids, att_pieces, ret_pieces, out_own, out_line, slots)
        sent = swap(parts[1], "tp")
        summed = (parts[0].astype(F32) + sent.astype(F32)).astype(BF16)
        pieces = [pick(summed, me, 1)]
        for k in range(1, MEMBERS):
            pieces.append(swap(pick(summed, me ^ k, 1), "si", k))
        groups.append(pieces)
    mixed = place(ids, groups)

    logs = jnp.transpose(logs).reshape(group, MEMBERS, tok_rows)
    log_weight = jnp.zeros((MEMBERS, group, tok_rows), F32)
    for k in range(MEMBERS):
        piece = pick(logs, me ^ k, 1)
        piece = piece if k == 0 else swap(piece, "si", k)
        log_weight = lax.dynamic_update_index_in_dim(log_weight, piece, me ^ k, 0)
    return (mixed, log_weight.reshape(heads, tok_rows))


def solution(mesh):
    sp, tp = mesh.shape["sp"], mesh.shape["tp"]

    def run(*args):
        members = args[3].shape[1] // HEAD_DIM // tp
        planes = sp // max(members, 1)
        fits = (
            (members, planes, tp) == (MEMBERS, PLANES, HALVES)
            and sp == members * planes
            and args[5].shape[1] == args[3].shape[1]
            and args[0].shape[0] // sp % CHUNK == 0
        )
        if not fits:
            split, body, names = mesh, shards, ("sp",)
        else:
            names = ("so", "si")
            split = Mesh(mesh.devices.reshape(planes, members, tp), names + ("tp",))
            body = plane_shards
        rows = P(names, "tp")
        cols = P("tp", names)
        return jax.shard_map(
            body,
            mesh=split,
            in_specs=(rows, P("tp")) + (rows,) * 6 + (cols, cols, P("tp"), cols),
            out_specs=(P(names + ("tp",), None), cols),
            check_vma=False,
        )(*args)

    return run
```
